32 devices in a mesh: sp: 8 (over z, x), tp: 4 (over y, core).
Axes of the slice: x: 2, y: 2, z: 4, core: 2. Of those that a mesh axis runs over, the one named last changes fastest.
Arguments:
- stream: bfloat16 [4096, 2048], P(('sp', 'tp')), may hold values from -6 to 6
- projected: bfloat16 [4096, 2048], P('sp', 'tp'), may hold values from -6 to 6
- segments: int32 [4096], P('sp'), may hold values from 0 to 3, never falling along the last dimension, each value on 1 to 1536 neighbouring positions
- group_weight: bfloat16 [4, 512, 512], replicated, may hold values from -0.25 to 0.25
- group_scale: float32 [2048], replicated, may hold values from 0.1 to 1.9
- out_weight: bfloat16 [2048, 2048], replicated, may hold values from -0.125 to 0.125
- ffn_gain: float32 [2048], replicated, may hold values from 0.1 to 1.9
- routes: int32 [4096, 4], P(('sp', 'tp')), may hold values from 0 to 31, all different within a row; in each aligned block of 128 rows (0 to 127, 128 to 255, ...) at most 24 rows name the same one
- route_weights: float32 [4096, 4], P(('sp', 'tp')), may hold values from 0.05 to 0.5
- expert_gate: bfloat16 [32, 2048, 1024], P(('sp', 'tp')), may hold values from -0.25 to 0.25
- expert_up: bfloat16 [32, 2048, 1024], P(('sp', 'tp')), may hold values from -0.25 to 0.25
- expert_down: bfloat16 [32, 1024, 2048], P(('sp', 'tp')), may hold values from -0.1875 to 0.1875
Outputs:
- combined: bfloat16 [4096, 2048], P(('sp', 'tp'))
The draws below stay inside these ranges and needn't reach their ends.
Inputs may be any that keep to these rules, and one draw needn't show every extreme that they name: `segments`: document numbers never fall along the positions; a document has 1 to 1536 positions, and one has exactly 1536. `routes`: each row names 4 different experts. Among the 128 rows of one device (aligned blocks), no expert is named more than 24 times, and in some blocks one is named exactly 24 times.
All inputs are finite; a program needn't handle non-finite values.
Results may differ from the reference program's by a relative error of at most 0.015.
Values may be sent and summed in bfloat16 or wider, within the bound.
A program may use at most 128 MiB of HBM per device.

```python
import math
import jax
import jax.numpy as jnp
import numpy as np
from jax import lax

D = 2048
GROUPS = 4
FF = 1024
TOP = 4
TOK_DEV = 128
TOKENS = 4096
GROUP_WIDTH = 512
EXPERTS = 32
CAP = 24
DOCS = 4
DOC_MOST = 1536


def levels(key, extent, shards, low, high):
    def one(dim, shards_of):
        heights = jax.random.uniform(jax.random.fold_in(jax.random.fold_in(key, 6), dim), (shards_of,), jnp.float32, low / len(shards), high / len(shards))
        return jnp.repeat(jnp.exp(heights), extent[dim] // shards_of).reshape((-1,) + (1,) * (len(extent) - dim - 1))

    loudness = one(*shards[0])
    for cut in shards[1:]:
        loudness = loudness * one(*cut)
    return loudness


def split_up(count, total, bound, skew):
    loads = [(1 << 20) // math.isqrt(standing ** skew) + 1 for standing in range(2, count + 1)]
    rest, given = total - bound - (count - 1), [1] * (count - 1)
    while rest > 0:
        candidates = [i for i in range(count - 1) if given[i] < bound]
        pool, remaining = sum([loads[i] for i in candidates]), rest
        for i in candidates:
            extra = min(bound - given[i], max(1, remaining * loads[i] // pool), rest)
            given[i] = given[i] + extra
            rest = rest - extra
    return np.array([bound] + given)


def ragged_sizes(own_key, number_of, total, most, skew):
    if number_of == 2:
        one = jax.random.randint(own_key, (), max(1, total - most), min(most, total - 1) + 1)
        return jnp.stack([one, total - one])
    lengths = jnp.asarray(split_up(number_of, total, most, skew), jnp.int32)
    couples = (number_of - 1) // 2
    source_of, taker = lengths[1:1 + 2 * couples:2], lengths[2:2 + 2 * couples:2]
    room = jnp.minimum(source_of - 1, most - taker)
    passed = jax.random.randint(jax.random.fold_in(own_key, 1), (couples,), 0, 1 << 20) % (room + 1)
    lengths = lengths.at[1:1 + 2 * couples:2].set(source_of - passed).at[2:2 + 2 * couples:2].set(taker + passed)
    return lengths[jax.random.permutation(jax.random.fold_in(own_key, 2), number_of)]


def deal_out(own_key, own, number, rows, number_of, top, most, lean):
    ranking = jax.random.permutation(own_key, number_of)
    crowded, usual = load_shares(number_of, rows * top, most, lean, True), load_shares(number_of, rows * top, most, lean, False)
    places = jnp.arange(number_of)

    def named(lengths, turn):
        used = int((lengths > 0).sum())
        fixed = max(1, used // 4)
        passed = fixed + (places - fixed + turn * (used - fixed)) % max(1, number_of - fixed)
        return jnp.zeros((number_of,), jnp.int32).at[ranking[jnp.where(places < fixed, places, passed)]].set(jnp.asarray(lengths, jnp.int32))

    lengths = jnp.where(number % 4 == 0, named(crowded, number // 4), named(usual, number - number // 4 - 1))
    mixed = jax.random.permutation(jax.random.fold_in(own, 3), number_of)
    giver, taker = mixed[0:number_of // 2 * 2:2], mixed[1:number_of // 2 * 2:2]
    margin = jnp.minimum(lengths[giver] - 1, most - lengths[taker]) // 2
    margin = jnp.where((giver == ranking[0]) | (taker == ranking[0]) | (lengths[taker] == 0), 0, jnp.maximum(margin, 0))
    passed = jax.random.randint(jax.random.fold_in(own, 4), (number_of // 2,), 0, 1 << 20) % (margin + 1)
    lengths = lengths.at[giver].add(-passed).at[taker].add(passed)
    labels = jnp.searchsorted(jnp.cumsum(lengths), jnp.arange(rows * top), side="right").astype(jnp.int32)
    table = labels.reshape(top, rows).T
    table = table[jax.random.permutation(jax.random.fold_in(own, 1), rows)]
    turn = jax.random.randint(jax.random.fold_in(own, 2), (rows, 1), 0, top)
    return jnp.take_along_axis(table, (jnp.arange(top)[None, :] + turn) % top, axis=1)


def load_shares(count, total, limit, skew, full):
    weights = [(1 << 20) // math.isqrt(rank ** skew) + 1 for rank in range(1, count + 1)]
    largest = limit if full else min(limit, max(-(-total // count), total * weights[0] // sum(weights)))
    least = 1 if total - largest >= count - 1 else 0
    holding, rest = [largest] + [least] * (count - 1), total - largest - least * (count - 1)
    while rest > 0:
        candidates = [i for i in range(1, count) if holding[i] < largest] or [i for i in range(1, count) if holding[i] < limit]
        pool, remaining = sum([weights[i] for i in candidates]), rest
        for i in candidates:
            addition = min(limit - holding[i], max(1, remaining * weights[i] // pool), rest)
            holding[i] = holding[i] + addition
            rest = rest - addition
    return np.array(holding)


def centred(stream_key, dims, spread, limit, cuts=(), kind=jnp.bfloat16):
    entries = spread * jax.random.normal(stream_key, dims, jnp.float32)
    if cuts:
        entries = entries * levels(stream_key, dims, cuts, -0.22, 0.18)
    return jnp.clip(entries, -limit, limit).astype(kind)


def setup_inputs(seed: int = 0) -> dict:
    streams_of = jax.random.split(jax.random.key(seed), 13)
    stream = centred(streams_of[0], (TOKENS, D), 1.0, 6.0, ((0, 32),))
    projected = centred(streams_of[1], (TOKENS, D), 1.0, 6.0, ((0, 8), (1, 4)))
    segments = jnp.searchsorted(jnp.cumsum(ragged_sizes(streams_of[2], DOCS, TOKENS, DOC_MOST, 2)), jnp.arange(TOKENS), side="right").astype(jnp.int32)
    group_weight = centred(streams_of[3], (GROUPS, GROUP_WIDTH, GROUP_WIDTH), GROUP_WIDTH ** -0.5, 0.25)
    group_scale = jnp.clip(1.0 + 0.18 * jax.random.normal(streams_of[4], (D,), jnp.float32), 0.1, 1.9)
    out_weight = centred(streams_of[5], (D, D), D ** -0.5, 0.125)
    ffn_gain = jnp.clip(1.0 + 0.18 * jax.random.normal(streams_of[6], (D,), jnp.float32), 0.1, 1.9)
    routes_keys = jax.random.split(jax.random.fold_in(streams_of[7], 1), TOKENS // TOK_DEV)
    routes_turns = jax.random.permutation(jax.random.fold_in(streams_of[7], 3), TOKENS // TOK_DEV)
    routes = jax.vmap(lambda own, number: deal_out(jax.random.fold_in(streams_of[7], 2), own, number, TOK_DEV, EXPERTS, TOP, CAP, 2))(routes_keys, routes_turns).reshape((TOKENS, TOP))
    route_weights = jnp.clip(0.05 + 0.45 * jax.random.uniform(streams_of[8], (TOKENS, TOP), jnp.float32) ** levels(streams_of[8], (TOKENS, TOP), ((0, 32),), -0.2, 0.2), 0.05, 0.5)
    expert_gate = centred(streams_of[9], (EXPERTS, D, FF), (D // 4) ** -0.5, 0.25, ((0, 32),))
    expert_up = centred(streams_of[10], (EXPERTS, D, FF), (D // 4) ** -0.5, 0.25, ((0, 32),))
    expert_down = centred(streams_of[11], (EXPERTS, FF, D), FF ** -0.5, 0.1875, ((0, 32),))
    return {"stream": stream, "projected": projected, "segments": segments, "group_weight": group_weight, "group_scale": group_scale, "out_weight": out_weight, "ffn_gain": ffn_gain, "routes": routes, "route_weights": route_weights, "expert_gate": expert_gate, "expert_up": expert_up, "expert_down": expert_down}


norm_eps = 1e-05
clamp_limit = 7.0
sigmoid_alpha = 1.702
longest_window = 16

def pool_residue(projected, segments):
    length, channels = projected.shape
    values = projected.astype(jnp.float32)
    channel = jnp.arange(channels, dtype=jnp.int32)
    window = jnp.left_shift(jnp.full((channels,), 2, jnp.int32), channel // (channels // GROUPS))
    window_sum = jnp.zeros((length, channels), jnp.float32)
    window_count = jnp.zeros((length, channels), jnp.float32)
    for offset in range(longest_window):
        earlier_rows = jnp.pad(values, ((offset, 0), (0, 0)))[:length]
        earlier_docs = jnp.pad(segments, (offset, 0), constant_values=-1)[:length]
        included = (earlier_docs == segments)[:, None] & (offset < window)[None, :]
        window_sum = window_sum + jnp.where(included, earlier_rows, jnp.float32(0.0))
        window_count = window_count + included.astype(jnp.float32)
    return (window_sum / window_count - values).astype(jnp.bfloat16)

def rms_scale(resid, gain):
    values = resid.astype(jnp.float32)
    inverse = lax.rsqrt(lax.optimization_barrier(jnp.mean(values * values, -1, keepdims=True)) + norm_eps)
    return (values * inverse * gain.astype(jnp.float32)).astype(jnp.bfloat16)

def run_expert(block, gate_matrix, up_matrix, down_matrix):
    leading = block.shape[:-1]
    flat_rows = block.reshape(-1, block.shape[-1])
    gate_value = jnp.dot(flat_rows, gate_matrix, preferred_element_type=jnp.float32)
    up_value = jnp.dot(flat_rows, up_matrix, preferred_element_type=jnp.float32)
    gated = jnp.minimum(gate_value, clamp_limit)
    linear = jnp.clip(up_value, -clamp_limit, clamp_limit)
    activated = (gated * jax.nn.sigmoid(sigmoid_alpha * gated) * (linear + 1.0)).astype(jnp.bfloat16)
    result = jnp.dot(activated, down_matrix, preferred_element_type=jnp.float32).astype(jnp.bfloat16)
    return result.reshape(leading + (down_matrix.shape[1],))

def reference(stream, projected, segments, group_weight, group_scale, out_weight, ffn_gain, routes, route_weights, expert_gate, expert_up, expert_down):
    mixed = pool_residue(projected, segments)
    length, model_width = mixed.shape
    group_width = model_width // GROUPS
    grouped = jnp.einsum('rgc,gcd->rgd', mixed.reshape(length, GROUPS, group_width).astype(jnp.float32), group_weight.astype(jnp.float32)).reshape(length, model_width)
    scaled = (grouped * group_scale.astype(jnp.float32)).astype(jnp.bfloat16)
    mixer_out = jnp.dot(scaled, out_weight, preferred_element_type=jnp.float32)
    resid = (stream.astype(jnp.float32) + mixer_out).astype(jnp.bfloat16)
    normed = rms_scale(resid, ffn_gain)
    flat_routes = routes.reshape(-1)
    flat_weights = route_weights.reshape(-1)
    token_of = jnp.arange(flat_routes.shape[0], dtype=jnp.int32) // TOP
    most_rows = EXPERTS * CAP

    def one_expert(carry, inputs):
        expert_id, gate_matrix, up_matrix, down_matrix = inputs
        matches = flat_routes == expert_id
        picked = jnp.nonzero(matches, size=most_rows, fill_value=0)[0].astype(jnp.int32)
        live = jnp.arange(most_rows, dtype=jnp.int32) < jnp.sum(matches.astype(jnp.int32))
        tokens_in = token_of[picked]
        expert_out = run_expert(normed[tokens_in], gate_matrix, up_matrix, down_matrix)
        weighting = jnp.where(live, flat_weights[picked], jnp.float32(0.0))
        carry = carry.at[tokens_in].add(expert_out.astype(jnp.float32) * weighting[:, None])
        return (carry, None)
    moe_sum, unused = lax.scan(one_expert, jnp.zeros((length, model_width), jnp.float32), (jnp.arange(EXPERTS, dtype=jnp.int32), expert_gate, expert_up, expert_down))
    return (resid.astype(jnp.float32) + moe_sum).astype(jnp.bfloat16)
```

```python
import jax
import jax.numpy as jnp
from jax import lax
from jax.experimental import pallas as pl
from jax.experimental.pallas import tpu as pltpu
from jax.sharding import PartitionSpec as P

GROUPS = 4


norm_eps = 1e-05
clamp_limit = 7.0
sigmoid_alpha = 1.702
longest_window = 16


def pool_kernel(group_width, halo_ref, rows_ref, docs_ref, mixed_ref):
    channels = rows_ref.shape[1]
    first = lax.axis_index("tp") * channels
    docs = docs_ref[...]
    same = [docs == pltpu.roll(docs, 1 << k, 0) for k in range(GROUPS)]
    for lane in range(0, channels, 128):
        cols = slice(lane, lane + 128)
        values = jnp.concatenate([halo_ref[:, cols], rows_ref[:, cols]], 0).astype(jnp.float32)
        total, count = values, jnp.ones_like(values)
        channel = first + lane + lax.broadcasted_iota(jnp.int32, values.shape, 1)
        for k in range(GROUPS):
            joins = same[k] & (channel >= k * group_width)
            total = jnp.where(joins, total + pltpu.roll(total, 1 << k, 0), total)
            count = jnp.where(joins, count + pltpu.roll(count, 1 << k, 0), count)
        mixed_ref[:, cols] = (total / count - values)[longest_window:].astype(jnp.bfloat16)


def pool(projected, segments, group_width):
    sp_count = lax.axis_size("sp")
    row_count, channels = projected.shape
    onward = [(i, i + 1) for i in range(sp_count - 1)]
    halo = lax.ppermute(projected[row_count - longest_window :], "sp", onward)
    halo_docs = lax.ppermute(segments[row_count - longest_window :], "sp", onward)
    halo_docs = jnp.where(lax.axis_index("sp") == 0, -1, halo_docs)
    docs = jnp.concatenate([halo_docs, segments])
    docs = jnp.broadcast_to(docs[:, None], (row_count + longest_window, 128))
    return pl.pallas_call(
        lambda *refs: pool_kernel(group_width, *refs),
        out_shape=jax.ShapeDtypeStruct((row_count, channels), jnp.bfloat16),
        name="pool",
    )(halo, projected, docs)


def slots_of(routes, expert_count, capacity):
    tok_count = routes.shape[0]
    named = routes[:, :, None] == jnp.arange(expert_count, dtype=jnp.int32)
    marks = jnp.sum(named.astype(jnp.float32), 1).astype(jnp.bfloat16)
    at = jnp.arange(tok_count, dtype=jnp.int32)
    earlier = (at[None, :] < at[:, None]).astype(jnp.bfloat16)
    before = jnp.dot(earlier, marks, preferred_element_type=jnp.float32)
    rank = jnp.sum(jnp.where(named, before[:, None, :], 0.0), 2).astype(jnp.int32)
    return routes * capacity + rank


def rms_scale(resid, gain):
    values = resid.astype(jnp.float32)
    inverse = lax.rsqrt(jnp.mean(values * values, -1, keepdims=True) + norm_eps)
    return (values * inverse * gain).astype(jnp.bfloat16)


def mixer(mixed, stream, group_weight, group_scale, out_weight, ffn_gain):
    tokens_here = lax.all_to_all(mixed, "tp", split_axis=0, concat_axis=1, tiled=True)
    group_width = group_weight.shape[1]
    grouped = jnp.concatenate(
        [
            jnp.dot(
                tokens_here[:, g * group_width : (g + 1) * group_width],
                group_weight[g],
                preferred_element_type=jnp.float32,
            )
            for g in range(GROUPS)
        ],
        1,
    )
    scaled = (grouped * group_scale).astype(jnp.bfloat16)
    mixer_out = jnp.dot(scaled, out_weight, preferred_element_type=jnp.float32)
    resid = (stream.astype(jnp.float32) + mixer_out).astype(jnp.bfloat16)
    return resid, rms_scale(resid, ffn_gain)


def run_expert(rows, gate_matrix, up_matrix, down_matrix):
    gate_value = jnp.dot(rows, gate_matrix, preferred_element_type=jnp.float32)
    up_value = jnp.dot(rows, up_matrix, preferred_element_type=jnp.float32)
    gated = jnp.minimum(gate_value, clamp_limit)
    linear = jnp.clip(up_value, -clamp_limit, clamp_limit)
    activated = (gated * jax.nn.sigmoid(sigmoid_alpha * gated) * (linear + 1.0)).astype(
        jnp.bfloat16
    )
    return jnp.dot(activated, down_matrix, preferred_element_type=jnp.float32).astype(jnp.bfloat16)


def body(
    stream,
    projected,
    segments,
    group_weight,
    group_scale,
    out_weight,
    ffn_gain,
    routes,
    route_weights,
    expert_gate,
    expert_up,
    expert_down,
):
    tok_count, model_width = stream.shape
    expert_count = lax.axis_size("sp") * lax.axis_size("tp")
    top_count = routes.shape[1]
    capacity = 3 * tok_count * top_count // (2 * expert_count)
    mixed = pool(projected, segments, group_weight.shape[1])
    slots = slots_of(routes, expert_count, capacity)
    resid, normed = mixer(mixed, stream, group_weight, group_scale, out_weight, ffn_gain)
    slot_ids = jnp.arange(expert_count * capacity, dtype=jnp.int32)
    chosen = slots[:, :, None] == slot_ids
    select = jnp.any(chosen, 1).astype(jnp.bfloat16)
    weigh = jnp.sum(jnp.where(chosen, route_weights[:, :, None], 0.0), 1).astype(jnp.bfloat16)
    outgoing = lax.dot_general(
        select, normed, (((0,), (0,)), ((), ())), preferred_element_type=jnp.float32
    ).astype(jnp.bfloat16)

    def exchange(rows):
        return lax.all_to_all(
            rows.reshape(expert_count, capacity, model_width),
            ("sp", "tp"),
            split_axis=0,
            concat_axis=0,
            tiled=True,
        ).reshape(expert_count * capacity, model_width)

    results = run_expert(exchange(outgoing), expert_gate[0], expert_up[0], expert_down[0])
    moe_sum = jnp.dot(weigh, exchange(results), preferred_element_type=jnp.float32)
    return (resid.astype(jnp.float32) + moe_sum).astype(jnp.bfloat16)


def solution(mesh):
    in_specs = (
        P(("sp", "tp"), None),
        P("sp", "tp"),
        P("sp"),
        P(),
        P(),
        P(),
        P(),
        P(("sp", "tp"), None),
        P(("sp", "tp"), None),
        P(("sp", "tp"), None, None),
        P(("sp", "tp"), None, None),
        P(("sp", "tp"), None, None),
    )
    out_specs = P(("sp", "tp"), None)
    return jax.shard_map(body, mesh=mesh, in_specs=in_specs, out_specs=out_specs, check_vma=False)
```

```python
import jax
import jax.numpy as jnp
from jax import lax
from jax.experimental import pallas as pl
from jax.experimental.pallas import tpu as pltpu
from jax.sharding import PartitionSpec as P

GROUPS = 4


norm_eps = 1e-05
clamp_limit = 7.0
sigmoid_alpha = 1.702
longest_window = 16


def pool_kernel(group_width, halo_ref, rows_ref, docs_ref, mixed_ref):
    channels = rows_ref.shape[1]
    first = lax.axis_index("tp") * channels
    docs = docs_ref[...]
    same = [docs == pltpu.roll(docs, 1 << k, 0) for k in range(GROUPS)]
    for lane in range(0, channels, 128):
        cols = slice(lane, lane + 128)
        values = jnp.concatenate([halo_ref[:, cols], rows_ref[:, cols]], 0).astype(jnp.float32)
        total, count = values, jnp.ones_like(values)
        channel = first + lane + lax.broadcasted_iota(jnp.int32, values.shape, 1)
        for k in range(GROUPS):
            joins = same[k] & (channel >= k * group_width)
            total = jnp.where(joins, total + pltpu.roll(total, 1 << k, 0), total)
            count = jnp.where(joins, count + pltpu.roll(count, 1 << k, 0), count)
        mixed_ref[:, cols] = (total / count - values)[longest_window:].astype(jnp.bfloat16)


def pool(projected, segments, group_width):
    sp_count = lax.axis_size("sp")
    row_count, channels = projected.shape
    onward = [(i, i + 1) for i in range(sp_count - 1)]
    halo = lax.ppermute(projected[row_count - longest_window :], "sp", onward)
    halo_docs = lax.ppermute(segments[row_count - longest_window :], "sp", onward)
    halo_docs = jnp.where(lax.axis_index("sp") == 0, -1, halo_docs)
    docs = jnp.concatenate([halo_docs, segments])
    docs = jnp.broadcast_to(docs[:, None], (row_count + longest_window, 128))
    return pl.pallas_call(
        lambda *refs: pool_kernel(group_width, *refs),
        out_shape=jax.ShapeDtypeStruct((row_count, channels), jnp.bfloat16),
        name="pool",
    )(halo, projected, docs)


def slots_of(routes, expert_count, capacity):
    tok_count = routes.shape[0]
    named = routes[:, :, None] == jnp.arange(expert_count, dtype=jnp.int32)
    marks = jnp.sum(named.astype(jnp.float32), 1).astype(jnp.bfloat16)
    at = jnp.arange(tok_count, dtype=jnp.int32)
    earlier = (at[None, :] < at[:, None]).astype(jnp.bfloat16)
    before = jnp.dot(earlier, marks, preferred_element_type=jnp.float32)
    rank = jnp.sum(jnp.where(named, before[:, None, :], 0.0), 2).astype(jnp.int32)
    return routes * capacity + rank


def rms_scale(resid, gain):
    values = resid.astype(jnp.float32)
    inverse = lax.rsqrt(jnp.mean(values * values, -1, keepdims=True) + norm_eps)
    return (values * inverse * gain).astype(jnp.bfloat16)


def mixer(mixed, stream, group_weight, group_scale, out_weight, ffn_gain):
    tokens_here = lax.all_to_all(mixed, "tp", split_axis=0, concat_axis=1, tiled=True)
    group_width = group_weight.shape[1]
    grouped = jnp.concatenate(
        [
            jnp.dot(
                tokens_here[:, g * group_width : (g + 1) * group_width],
                group_weight[g],
                preferred_element_type=jnp.float32,
            )
            for g in range(GROUPS)
        ],
        1,
    )
    scaled = (grouped * group_scale).astype(jnp.bfloat16)
    mixer_out = jnp.dot(scaled, out_weight, preferred_element_type=jnp.float32)
    resid = (stream.astype(jnp.float32) + mixer_out).astype(jnp.bfloat16)
    return resid, rms_scale(resid, ffn_gain)


CHUNKS = 4


def experts_kernel(
    z_count,
    x_count,
    tp_count,
    normed_ref,
    resid_ref,
    select_ref,
    weigh_ref,
    gate_hbm,
    up_hbm,
    down_hbm,
    out_ref,
    gate_ref,
    up_ref,
    down_ref,
    column,
    outgoing,
    rows,
    gate_sum,
    up_sum,
    activated,
    results,
    returned,
    part,
    right_out,
    left_out,
    right_in,
    left_in,
    load_sem,
    col_send,
    col_recv,
    plane_send,
    plane_recv,
    back_send,
    back_recv,
    sum_send,
    sum_recv,
):
    sp, tp = lax.axis_index("sp"), lax.axis_index("tp")
    z, x = lax.div(sp, x_count), lax.rem(sp, x_count)
    plane = x_count * tp_count
    place = x * tp_count + tp
    tok, width = normed_ref.shape
    wide = width // CHUNKS
    share = select_ref.shape[0] // plane
    tile = min(256, wide)
    last = z_count - 1
    has_right, has_left = z < last, z > 0

    def at_z(step):
        return {"sp": sp + step * x_count, "tp": tp}

    def at_plane(other):
        return {"sp": z * x_count + lax.div(other, tp_count), "tp": lax.rem(other, tp_count)}

    def remote(src, dst, send, recv, device):
        return pltpu.make_async_remote_copy(
            src_ref=src,
            dst_ref=dst,
            send_sem=send,
            recv_sem=recv,
            device_id=device,
            device_id_type=pl.DeviceIdType.MESH,
        )

    def cols_of(k):
        return pl.ds(pl.multiple_of(k * wide, wide), wide)

    def share_of(i):
        return pl.ds(pl.multiple_of(i * share, share), share)

    loads = [
        pltpu.make_async_copy(src, dst, load_sem.at[i])
        for i, (src, dst) in enumerate(
            ((gate_hbm, gate_ref), (up_hbm, up_ref), (down_hbm, down_ref))
        )
    ]

    barrier = pltpu.get_barrier_semaphore()

    def greet(device):
        pl.semaphore_signal(barrier, inc=1, device_id=device, device_id_type=pl.DeviceIdType.MESH)

    pl.when(has_right)(lambda: greet(at_z(1)))
    pl.when(has_left)(lambda: greet(at_z(-1)))

    @pl.loop(1, plane)
    def _(i):
        greet(at_plane(lax.rem(place + i, plane)))

    for load in loads:
        load.start()
    gate_sum[...] = jnp.zeros_like(gate_sum)
    up_sum[...] = jnp.zeros_like(up_sum)
    pl.semaphore_wait(
        barrier, plane - 1 + has_right.astype(jnp.int32) + has_left.astype(jnp.int32)
    )

    def to_right(k, e):
        src = normed_ref.at[:, cols_of(k)] if e == 0 else column.at[k, e - 1]
        return remote(
            src, column.at[k, e], col_send.at[k, 0, e], col_recv.at[k, e], at_z(1)
        )

    def to_left(k, e):
        src = normed_ref.at[:, cols_of(k)] if e == 0 else column.at[k, z_count - e - 1]
        back = z_count - e - 2
        return remote(
            src, column.at[k, back], col_send.at[k, 1, e], col_recv.at[k, back], at_z(-1)
        )

    def send_own(k):
        pl.when(has_right)(lambda: to_right(k, 0).start())
        pl.when(has_left)(lambda: to_left(k, 0).start())

    def relay(k):
        for e in range(1, z_count):

            @pl.when(z >= e)
            def _():
                to_right(k, e - 1).wait_recv()
                if e < last:
                    pl.when(has_right)(lambda: to_right(k, e).start())

            @pl.when(last - z >= e)
            def _():
                to_left(k, e - 1).wait_recv()
                if e < last:
                    pl.when(has_left)(lambda: to_left(k, e).start())

    def to_expert(k, i):
        other = lax.rem(place + i, plane)
        return remote(
            outgoing.at[k, share_of(other)],
            rows.at[k, share_of(i)],
            plane_send.at[k, i - 1],
            plane_recv.at[k, i - 1],
            at_plane(other),
        )

    def dispatch(k):
        own = jnp.dot(
            select_ref[:, :tok], normed_ref[:, cols_of(k)], preferred_element_type=jnp.float32
        )
        others = jnp.dot(
            select_ref[:, tok:],
            column[k].reshape(last * tok, wide),
            preferred_element_type=jnp.float32,
        )
        outgoing[k] = (own + others).astype(jnp.bfloat16)

        @pl.loop(1, plane)
        def _(i):
            to_expert(k, i).start()

        rows[k, pl.ds(0, share)] = outgoing[k, share_of(place)]

    def accumulate(k):
        @pl.loop(1, plane)
        def _(i):
            to_expert(k, i).wait_recv()

        @pl.loop(0, gate_ref.shape[1] // tile)
        def _(n):
            cols = pl.ds(pl.multiple_of(n * tile, tile), tile)
            gate_sum[:, cols] += jnp.dot(
                rows[k], gate_ref[cols_of(k), cols], preferred_element_type=jnp.float32
            )
            up_sum[:, cols] += jnp.dot(
                rows[k], up_ref[cols_of(k), cols], preferred_element_type=jnp.float32
            )

    send_own(0)

    @pl.loop(0, CHUNKS)
    def _(k):
        pl.when(k + 1 < CHUNKS)(lambda: send_own(k + 1))
        relay(k)
        dispatch(k)

        @pl.when(k == 1)
        def _():
            loads[0].wait()
            loads[1].wait()

        pl.when(k > 0)(lambda: accumulate(k - 1))

    accumulate(CHUNKS - 1)

    @pl.loop(0, gate_ref.shape[1] // tile)
    def _(n):
        cols = pl.ds(pl.multiple_of(n * tile, tile), tile)
        gated = jnp.minimum(gate_sum[:, cols], clamp_limit)
        linear = jnp.clip(up_sum[:, cols], -clamp_limit, clamp_limit)
        activated[:, cols] = (
            gated * jax.nn.sigmoid(sigmoid_alpha * gated) * (linear + 1.0)
        ).astype(jnp.bfloat16)

    loads[2].wait()

    def to_relay(k, i):
        return remote(
            results.at[k, share_of(i)],
            returned.at[k, share_of(place)],
            back_send.at[k, i - 1],
            back_recv.at[k, i - 1],
            at_plane(lax.rem(place + plane - i, plane)),
        )

    @pl.loop(0, CHUNKS)
    def _(k):
        @pl.loop(0, wide // tile)
        def _(n):
            cols = pl.ds(pl.multiple_of(n * tile, tile), tile)
            from_cols = pl.ds(pl.multiple_of(k * wide + n * tile, tile), tile)
            results[k, :, cols] = jnp.dot(
                activated[...], down_ref[:, from_cols], preferred_element_type=jnp.float32
            ).astype(jnp.bfloat16)

        @pl.loop(1, plane)
        def _(i):
            to_relay(k, i).start()

        returned[k, share_of(place)] = results[k, pl.ds(0, share)]

    def combine(k):
        @pl.loop(1, plane)
        def _(i):
            to_relay(k, i).wait_recv()

        part[k] = jnp.dot(weigh_ref[...], returned[k], preferred_element_type=jnp.float32)

    def sum_right(k, e):
        return remote(
            right_out.at[k, e - 1],
            right_in.at[k, e - 1],
            sum_send.at[k, 0, e - 1],
            sum_recv.at[k, 0, e - 1],
            at_z(1),
        )

    def sum_left(k, e):
        return remote(
            left_out.at[k, e - 1],
            left_in.at[k, e - 1],
            sum_send.at[k, 1, e - 1],
            sum_recv.at[k, 1, e - 1],
            at_z(-1),
        )

    def add_up(k):
        for e in range(last, 0, -1):

            @pl.when(z + e <= last)
            def _():
                mine = slice((z_count - e) * tok, (z_count - e + 1) * tok)
                if e < last:

                    @pl.when(has_left)
                    def _():
                        sum_right(k, e + 1).wait_recv()
                        part[k, mine] += right_in[k, e].astype(jnp.float32)

                right_out[k, e - 1] = part[k, mine].astype(jnp.bfloat16)
                sum_right(k, e).start()

            @pl.when(z >= e)
            def _():
                mine = slice(e * tok, (e + 1) * tok)
                if e < last:

                    @pl.when(has_right)
                    def _():
                        sum_left(k, e + 1).wait_recv()
                        part[k, mine] += left_in[k, e].astype(jnp.float32)

                left_out[k, e - 1] = part[k, mine].astype(jnp.bfloat16)
                sum_left(k, e).start()

    def finish(k):
        own = slice(0, tok)

        @pl.when(has_left)
        def _():
            sum_right(k, 1).wait_recv()
            part[k, own] += right_in[k, 0].astype(jnp.float32)

        @pl.when(has_right)
        def _():
            sum_left(k, 1).wait_recv()
            part[k, own] += left_in[k, 0].astype(jnp.float32)

        out_ref[:, cols_of(k)] = (
            resid_ref[:, cols_of(k)].astype(jnp.float32) + part[k, own]
        ).astype(jnp.bfloat16)

    combine(0)

    @pl.loop(0, CHUNKS)
    def _(k):
        pl.when(k + 1 < CHUNKS)(lambda: combine(k + 1))
        add_up(k)
        pl.when(k > 0)(lambda: finish(k - 1))

    finish(CHUNKS - 1)

    @pl.loop(0, CHUNKS)
    def _(k):
        for e in range(last):

            @pl.when((z >= e) & has_right)
            def _():
                to_right(k, e).wait_send()

            @pl.when((last - z >= e) & has_left)
            def _():
                to_left(k, e).wait_send()

        for e in range(1, z_count):
            pl.when(z + e <= last)(lambda: sum_right(k, e).wait_send())
            pl.when(z >= e)(lambda: sum_left(k, e).wait_send())

        @pl.loop(1, plane)
        def _(i):
            to_expert(k, i).wait_send()
            to_relay(k, i).wait_send()


def run_experts(normed, resid, routes, route_weights, gate, up, down):
    tok, width = normed.shape
    sp_count, tp_count = lax.axis_size("sp"), lax.axis_size("tp")
    x_count = max(tp_count // 2, 1)
    z_count = sp_count // x_count
    plane = x_count * tp_count
    top_count = routes.shape[1]
    hidden = gate.shape[1]
    capacity = 3 * tok * top_count // (2 * plane * z_count)
    share = -(-z_count * capacity // 16) * 16
    slots = slots_of(routes, plane * z_count, capacity)
    info = jnp.concatenate([slots.astype(jnp.float32), route_weights], 1)
    z = lax.axis_index("sp") // x_count
    slot_ids = jnp.arange(plane * share, dtype=jnp.int32)
    targets, weights = [], []
    for d in range(z_count):
        here = info
        if d:
            onward = [(s, (s + d * x_count) % sp_count) for s in range(sp_count)]
            here = lax.ppermute(info, "sp", onward)
        local = here[:, :top_count].astype(jnp.int32) - z * plane * capacity
        inside = (local >= 0) & (local < plane * capacity)
        target = local // capacity * share + d * capacity + local % capacity
        targets.append(jnp.where(inside, target, -1))
        weights.append(here[:, top_count:])
    target, weight = jnp.concatenate(targets), jnp.concatenate(weights)
    target_t = target.T
    select, weigh = False, 0.0
    for j in range(top_count):
        select = select | (slot_ids[:, None] == target_t[j][None, :])
        weigh = weigh + jnp.where(target[:, j, None] == slot_ids[None, :], weight[:, j, None], 0.0)
    select, weigh = select.astype(jnp.bfloat16), weigh.astype(jnp.bfloat16)
    wide = width // CHUNKS
    last = z_count - 1
    bf, f32 = jnp.bfloat16, jnp.float32
    vmem = pl.BlockSpec(memory_space=pltpu.VMEM)
    hbm = pl.BlockSpec(memory_space=pl.ANY)
    dma = pltpu.SemaphoreType.DMA
    slab = pltpu.VMEM((CHUNKS, plane * share, wide), bf)
    hop = pltpu.VMEM((CHUNKS, last, tok, wide), bf)
    return pl.pallas_call(
        lambda *refs: experts_kernel(z_count, x_count, tp_count, *refs),
        out_shape=jax.ShapeDtypeStruct((tok, width), bf),
        in_specs=[vmem] * 4 + [hbm] * 3,
        out_specs=vmem,
        scratch_shapes=[
            pltpu.VMEM((width, hidden), bf),
            pltpu.VMEM((width, hidden), bf),
            pltpu.VMEM((hidden, width), bf),
            hop,
            slab,
            slab,
            pltpu.VMEM((plane * share, hidden), f32),
            pltpu.VMEM((plane * share, hidden), f32),
            pltpu.VMEM((plane * share, hidden), bf),
            slab,
            slab,
            pltpu.VMEM((CHUNKS, z_count * tok, wide), f32),
            hop,
            hop,
            hop,
            hop,
            dma((3,)),
            dma((CHUNKS, 2, last)),
            dma((CHUNKS, last)),
            dma((CHUNKS, plane - 1)),
            dma((CHUNKS, plane - 1)),
            dma((CHUNKS, plane - 1)),
            dma((CHUNKS, plane - 1)),
            dma((CHUNKS, 2, last)),
            dma((CHUNKS, 2, last)),
        ],
        compiler_params=pltpu.CompilerParams(
            collective_id=0, has_side_effects=True, vmem_limit_bytes=65000 * 1024
        ),
        name="experts",
    )(normed, resid, select, weigh, gate, up, down)


def body(
    stream,
    projected,
    segments,
    group_weight,
    group_scale,
    out_weight,
    ffn_gain,
    routes,
    route_weights,
    expert_gate,
    expert_up,
    expert_down,
):
    mixed = pool(projected, segments, group_weight.shape[1])
    resid, normed = mixer(mixed, stream, group_weight, group_scale, out_weight, ffn_gain)
    return run_experts(
        normed, resid, routes, route_weights, expert_gate[0], expert_up[0], expert_down[0]
    )


def solution(mesh):
    in_specs = (
        P(("sp", "tp"), None),
        P("sp", "tp"),
        P("sp"),
        P(),
        P(),
        P(),
        P(),
        P(("sp", "tp"), None),
        P(("sp", "tp"), None),
        P(("sp", "tp"), None, None),
        P(("sp", "tp"), None, None),
        P(("sp", "tp"), None, None),
    )
    out_specs = P(("sp", "tp"), None)
    return jax.shard_map(body, mesh=mesh, in_specs=in_specs, out_specs=out_specs, check_vma=False)
```

```python
import jax
import jax.numpy as jnp
from jax import lax
from jax.experimental import pallas as pl
from jax.experimental.pallas import tpu as pltpu
from jax.sharding import PartitionSpec as P

GROUPS = 4


norm_eps = 1e-05
clamp_limit = 7.0
sigmoid_alpha = 1.702
longest_window = 16


def pool_kernel(group_width, halo_ref, rows_ref, docs_ref, mixed_ref):
    channels = rows_ref.shape[1]
    first = lax.axis_index("tp") * channels
    docs = docs_ref[...]
    same = [docs == pltpu.roll(docs, 1 << k, 0) for k in range(GROUPS)]
    for lane in range(0, channels, 128):
        cols = slice(lane, lane + 128)
        values = jnp.concatenate([halo_ref[:, cols], rows_ref[:, cols]], 0).astype(jnp.float32)
        total, count = values, jnp.ones_like(values)
        channel = first + lane + lax.broadcasted_iota(jnp.int32, values.shape, 1)
        for k in range(GROUPS):
            joins = same[k] & (channel >= k * group_width)
            total = jnp.where(joins, total + pltpu.roll(total, 1 << k, 0), total)
            count = jnp.where(joins, count + pltpu.roll(count, 1 << k, 0), count)
        mixed_ref[:, cols] = (total / count - values)[longest_window:].astype(jnp.bfloat16)


def exchange_kernel(
    z_count, x_count, sp_count,
    tail_ref, docs_ref, info_ref, halo_ref, halo_docs_ref, infos_ref,
    halo, halo_docs, infos, send_sem, recv_sem,
):
    sp, tp = lax.axis_index("sp"), lax.axis_index("tp")
    z, x = lax.div(sp, x_count), lax.rem(sp, x_count)
    has_next, has_prev = sp < sp_count - 1, sp > 0
    barrier = pltpu.get_barrier_semaphore()

    def along_z(d):
        return {"sp": lax.rem(z + d, z_count) * x_count + x, "tp": tp}

    def along_sp(step):
        return {"sp": sp + step, "tp": tp}

    def greet(device):
        pl.semaphore_signal(barrier, inc=1, device_id=device, device_id_type=pl.DeviceIdType.MESH)

    def remote(src, dst, i, device):
        return pltpu.make_async_remote_copy(
            src_ref=src,
            dst_ref=dst,
            send_sem=send_sem.at[i],
            recv_sem=recv_sem.at[i],
            device_id=device,
            device_id_type=pl.DeviceIdType.MESH,
        )

    pl.when(has_next)(lambda: greet(along_sp(1)))
    pl.when(has_prev)(lambda: greet(along_sp(-1)))
    for d in range(1, z_count):
        greet(along_z(d))
    pl.semaphore_wait(
        barrier, z_count - 1 + has_next.astype(jnp.int32) + has_prev.astype(jnp.int32)
    )
    tables = [remote(info_ref, infos.at[d - 1], d + 1, along_z(d)) for d in range(1, z_count)]
    edges = [
        remote(tail_ref, halo, 0, along_sp(1)),
        remote(docs_ref, halo_docs, 1, along_sp(1)),
    ]

    @pl.when(has_next)
    def _():
        for copy in edges:
            copy.start()

    for copy in tables:
        copy.start()
    infos_ref[0] = info_ref[...]

    @pl.when(has_prev)
    def _():
        for copy in edges:
            copy.wait_recv()
        halo_ref[...] = halo[...]
        halo_docs_ref[...] = halo_docs[...]

    @pl.when(sp == 0)
    def _():
        halo_ref[...] = jnp.zeros_like(halo_ref)
        halo_docs_ref[...] = jnp.full_like(halo_docs_ref, -1)

    for d, copy in enumerate(tables):
        copy.wait_recv()
        infos_ref[d + 1] = infos[d]

    @pl.when(has_next)
    def _():
        for copy in edges:
            copy.wait_send()

    for copy in tables:
        copy.wait_send()


def exchange(projected, segments, routes, route_weights):
    row_count, channels = projected.shape
    sp_count, tp_count = lax.axis_size("sp"), lax.axis_size("tp")
    x_count = max(tp_count // 2, 1)
    z_count = sp_count // x_count
    tok, top_count = routes.shape
    capacity = 3 * tok * top_count // (2 * sp_count * tp_count)
    slots = slots_of(routes, sp_count * tp_count, capacity)
    info = jnp.concatenate([slots.astype(jnp.float32), route_weights], 1).T
    docs = jnp.broadcast_to(segments[:, None], (row_count, 128))
    edge = (longest_window, channels)
    halo, halo_docs, infos = pl.pallas_call(
        lambda *refs: exchange_kernel(z_count, x_count, sp_count, *refs),
        out_shape=(
            jax.ShapeDtypeStruct(edge, jnp.bfloat16),
            jax.ShapeDtypeStruct((longest_window, 128), jnp.int32),
            jax.ShapeDtypeStruct((z_count, 2 * top_count, tok), jnp.float32),
        ),
        in_specs=[pl.BlockSpec(memory_space=pltpu.VMEM)] * 3,
        out_specs=(pl.BlockSpec(memory_space=pltpu.VMEM),) * 3,
        scratch_shapes=[
            pltpu.VMEM(edge, jnp.bfloat16),
            pltpu.VMEM((longest_window, 128), jnp.int32),
            pltpu.VMEM((z_count - 1, 2 * top_count, tok), jnp.float32),
            pltpu.SemaphoreType.DMA((z_count + 1,)),
            pltpu.SemaphoreType.DMA((z_count + 1,)),
        ],
        compiler_params=pltpu.CompilerParams(collective_id=1, has_side_effects=True),
        name="exchange",
    )(projected[row_count - longest_window :], docs[row_count - longest_window :], info)
    return halo, jnp.concatenate([halo_docs, docs]), infos


def pool(projected, halo, docs, group_width):
    row_count, channels = projected.shape
    return pl.pallas_call(
        lambda *refs: pool_kernel(group_width, *refs),
        out_shape=jax.ShapeDtypeStruct((row_count, channels), jnp.bfloat16),
        name="pool",
    )(halo, projected, docs)


def slots_of(routes, expert_count, capacity):
    tok_count = routes.shape[0]
    named = routes[:, :, None] == jnp.arange(expert_count, dtype=jnp.int32)
    marks = jnp.sum(named.astype(jnp.float32), 1).astype(jnp.bfloat16)
    at = jnp.arange(tok_count, dtype=jnp.int32)
    earlier = (at[None, :] < at[:, None]).astype(jnp.bfloat16)
    before = jnp.dot(earlier, marks, preferred_element_type=jnp.float32)
    rank = jnp.sum(jnp.where(named, before[:, None, :], 0.0), 2).astype(jnp.int32)
    return routes * capacity + rank


def rms_scale(resid, gain):
    values = resid.astype(jnp.float32)
    inverse = lax.rsqrt(jnp.mean(values * values, -1, keepdims=True) + norm_eps)
    return (values * inverse * gain).astype(jnp.bfloat16)


def mixer(mixed, stream, group_weight, group_scale, out_weight, ffn_gain):
    tokens_here = lax.all_to_all(mixed, "tp", split_axis=0, concat_axis=1, tiled=True)
    group_width = group_weight.shape[1]
    grouped = jnp.concatenate(
        [
            jnp.dot(
                tokens_here[:, g * group_width : (g + 1) * group_width],
                group_weight[g],
                preferred_element_type=jnp.float32,
            )
            for g in range(GROUPS)
        ],
        1,
    )
    scaled = (grouped * group_scale).astype(jnp.bfloat16)
    mixer_out = jnp.dot(scaled, out_weight, preferred_element_type=jnp.float32)
    resid = (stream.astype(jnp.float32) + mixer_out).astype(jnp.bfloat16)
    return resid, rms_scale(resid, ffn_gain)


CHUNKS = 8


def experts_kernel(
    z_count,
    x_count,
    tp_count,
    normed_ref,
    resid_ref,
    select_ref,
    weigh_ref,
    gate_hbm,
    up_hbm,
    down_hbm,
    out_ref,
    gate_ref,
    up_ref,
    down_ref,
    column,
    outgoing,
    rows,
    gate_sum,
    up_sum,
    activated,
    results,
    returned,
    part,
    right_out,
    left_out,
    right_in,
    left_in,
    load_sem,
    col_send,
    col_recv,
    plane_send,
    plane_recv,
    back_send,
    back_recv,
    sum_send,
    sum_recv,
):
    sp, tp = lax.axis_index("sp"), lax.axis_index("tp")
    z, x = lax.div(sp, x_count), lax.rem(sp, x_count)
    plane = x_count * tp_count
    place = x * tp_count + tp
    tok, width = normed_ref.shape
    wide = width // CHUNKS
    share = select_ref.shape[0] // plane
    tile = min(256, wide)
    last = z_count - 1
    has_right, has_left = z < last, z > 0

    def at_z(step):
        return {"sp": sp + step * x_count, "tp": tp}

    def at_plane(other):
        return {"sp": z * x_count + lax.div(other, tp_count), "tp": lax.rem(other, tp_count)}

    def remote(src, dst, send, recv, device):
        return pltpu.make_async_remote_copy(
            src_ref=src,
            dst_ref=dst,
            send_sem=send,
            recv_sem=recv,
            device_id=device,
            device_id_type=pl.DeviceIdType.MESH,
        )

    def cols_of(k):
        return pl.ds(pl.multiple_of(k * wide, wide), wide)

    def share_of(i):
        return pl.ds(pl.multiple_of(i * share, share), share)

    loads = [
        pltpu.make_async_copy(src, dst, load_sem.at[i])
        for i, (src, dst) in enumerate(
            ((gate_hbm, gate_ref), (up_hbm, up_ref), (down_hbm, down_ref))
        )
    ]

    barrier = pltpu.get_barrier_semaphore()

    def greet(device):
        pl.semaphore_signal(barrier, inc=1, device_id=device, device_id_type=pl.DeviceIdType.MESH)

    pl.when(has_right)(lambda: greet(at_z(1)))
    pl.when(has_left)(lambda: greet(at_z(-1)))

    @pl.loop(1, plane)
    def _(i):
        greet(at_plane(lax.rem(place + i, plane)))

    for load in loads:
        load.start()
    gate_sum[...] = jnp.zeros_like(gate_sum)
    up_sum[...] = jnp.zeros_like(up_sum)
    pl.semaphore_wait(
        barrier, plane - 1 + has_right.astype(jnp.int32) + has_left.astype(jnp.int32)
    )

    def to_right(k, e):
        src = normed_ref.at[:, cols_of(k)] if e == 0 else column.at[k, e - 1]
        return remote(
            src, column.at[k, e], col_send.at[k, 0, e], col_recv.at[k, e], at_z(1)
        )

    def to_left(k, e):
        src = normed_ref.at[:, cols_of(k)] if e == 0 else column.at[k, z_count - e - 1]
        back = z_count - e - 2
        return remote(
            src, column.at[k, back], col_send.at[k, 1, e], col_recv.at[k, back], at_z(-1)
        )

    def send_own(k):
        pl.when(has_right)(lambda: to_right(k, 0).start())
        pl.when(has_left)(lambda: to_left(k, 0).start())

    def relay(k):
        for e in range(1, z_count):

            @pl.when(z >= e)
            def _():
                to_right(k, e - 1).wait_recv()
                if e < last:
                    pl.when(has_right)(lambda: to_right(k, e).start())

            @pl.when(last - z >= e)
            def _():
                to_left(k, e - 1).wait_recv()
                if e < last:
                    pl.when(has_left)(lambda: to_left(k, e).start())

    def to_expert(k, i):
        other = lax.rem(place + i, plane)
        return remote(
            outgoing.at[k, share_of(other)],
            rows.at[k, share_of(i)],
            plane_send.at[k, i - 1],
            plane_recv.at[k, i - 1],
            at_plane(other),
        )

    def dispatch(k):
        own = jnp.dot(
            select_ref[:, :tok], normed_ref[:, cols_of(k)], preferred_element_type=jnp.float32
        )
        others = jnp.dot(
            select_ref[:, tok:],
            column[k].reshape(last * tok, wide),
            preferred_element_type=jnp.float32,
        )
        outgoing[k] = (own + others).astype(jnp.bfloat16)

        @pl.loop(1, plane)
        def _(i):
            to_expert(k, i).start()

        rows[k, pl.ds(0, share)] = outgoing[k, share_of(place)]

    def accumulate(k):
        @pl.loop(1, plane)
        def _(i):
            to_expert(k, i).wait_recv()

        @pl.loop(0, gate_ref.shape[1] // tile)
        def _(n):
            cols = pl.ds(pl.multiple_of(n * tile, tile), tile)
            gate_sum[:, cols] += jnp.dot(
                rows[k], gate_ref[cols_of(k), cols], preferred_element_type=jnp.float32
            )
            up_sum[:, cols] += jnp.dot(
                rows[k], up_ref[cols_of(k), cols], preferred_element_type=jnp.float32
            )

    send_own(0)

    @pl.loop(0, CHUNKS)
    def _(k):
        pl.when(k + 1 < CHUNKS)(lambda: send_own(k + 1))
        relay(k)
        dispatch(k)

        @pl.when(k == 1)
        def _():
            loads[0].wait()
            loads[1].wait()

        pl.when(k > 0)(lambda: accumulate(k - 1))

    accumulate(CHUNKS - 1)

    @pl.loop(0, gate_ref.shape[1] // tile)
    def _(n):
        cols = pl.ds(pl.multiple_of(n * tile, tile), tile)
        gated = jnp.minimum(gate_sum[:, cols], clamp_limit)
        linear = jnp.clip(up_sum[:, cols], -clamp_limit, clamp_limit)
        activated[:, cols] = (
            gated * jax.nn.sigmoid(sigmoid_alpha * gated) * (linear + 1.0)
        ).astype(jnp.bfloat16)

    loads[2].wait()

    def to_relay(k, i):
        return remote(
            results.at[k, share_of(i)],
            returned.at[k, share_of(place)],
            back_send.at[k, i - 1],
            back_recv.at[k, i - 1],
            at_plane(lax.rem(place + plane - i, plane)),
        )

    @pl.loop(0, CHUNKS)
    def _(k):
        @pl.loop(0, wide // tile)
        def _(n):
            cols = pl.ds(pl.multiple_of(n * tile, tile), tile)
            from_cols = pl.ds(pl.multiple_of(k * wide + n * tile, tile), tile)
            results[k, :, cols] = jnp.dot(
                activated[...], down_ref[:, from_cols], preferred_element_type=jnp.float32
            ).astype(jnp.bfloat16)

        @pl.loop(1, plane)
        def _(i):
            to_relay(k, i).start()

        returned[k, share_of(place)] = results[k, pl.ds(0, share)]

    def combine(k):
        @pl.loop(1, plane)
        def _(i):
            to_relay(k, i).wait_recv()

        part[k] = jnp.dot(weigh_ref[...], returned[k], preferred_element_type=jnp.float32)

    def sum_right(k, e):
        return remote(
            right_out.at[k, e - 1],
            right_in.at[k, e - 1],
            sum_send.at[k, 0, e - 1],
            sum_recv.at[k, 0, e - 1],
            at_z(1),
        )

    def sum_left(k, e):
        return remote(
            left_out.at[k, e - 1],
            left_in.at[k, e - 1],
            sum_send.at[k, 1, e - 1],
            sum_recv.at[k, 1, e - 1],
            at_z(-1),
        )

    def add_up(k):
        for e in range(last, 0, -1):

            @pl.when(z + e <= last)
            def _():
                mine = slice((z_count - e) * tok, (z_count - e + 1) * tok)
                if e < last:

                    @pl.when(has_left)
                    def _():
                        sum_right(k, e + 1).wait_recv()
                        part[k, mine] += right_in[k, e].astype(jnp.float32)

                right_out[k, e - 1] = part[k, mine].astype(jnp.bfloat16)
                sum_right(k, e).start()

            @pl.when(z >= e)
            def _():
                mine = slice(e * tok, (e + 1) * tok)
                if e < last:

                    @pl.when(has_right)
                    def _():
                        sum_left(k, e + 1).wait_recv()
                        part[k, mine] += left_in[k, e].astype(jnp.float32)

                left_out[k, e - 1] = part[k, mine].astype(jnp.bfloat16)
                sum_left(k, e).start()

    def finish(k):
        own = slice(0, tok)

        @pl.when(has_left)
        def _():
            sum_right(k, 1).wait_recv()
            part[k, own] += right_in[k, 0].astype(jnp.float32)

        @pl.when(has_right)
        def _():
            sum_left(k, 1).wait_recv()
            part[k, own] += left_in[k, 0].astype(jnp.float32)

        out_ref[:, cols_of(k)] = (
            resid_ref[:, cols_of(k)].astype(jnp.float32) + part[k, own]
        ).astype(jnp.bfloat16)

    combine(0)

    @pl.loop(0, CHUNKS)
    def _(k):
        pl.when(k + 1 < CHUNKS)(lambda: combine(k + 1))
        add_up(k)
        pl.when(k > 0)(lambda: finish(k - 1))

    finish(CHUNKS - 1)

    @pl.loop(0, CHUNKS)
    def _(k):
        for e in range(last):

            @pl.when((z >= e) & has_right)
            def _():
                to_right(k, e).wait_send()

            @pl.when((last - z >= e) & has_left)
            def _():
                to_left(k, e).wait_send()

        for e in range(1, z_count):
            pl.when(z + e <= last)(lambda: sum_right(k, e).wait_send())
            pl.when(z >= e)(lambda: sum_left(k, e).wait_send())

        @pl.loop(1, plane)
        def _(i):
            to_expert(k, i).wait_send()
            to_relay(k, i).wait_send()


def run_experts(normed, resid, infos, gate, up, down):
    tok, width = normed.shape
    sp_count, tp_count = lax.axis_size("sp"), lax.axis_size("tp")
    x_count = max(tp_count // 2, 1)
    z_count = sp_count // x_count
    plane = x_count * tp_count
    top_count = infos.shape[1] // 2
    hidden = gate.shape[1]
    capacity = 3 * tok * top_count // (2 * plane * z_count)
    share = -(-z_count * capacity // 16) * 16
    z = lax.axis_index("sp") // x_count
    slot_ids = jnp.arange(plane * share, dtype=jnp.int32)
    local = infos[:, :top_count].astype(jnp.int32) - z * plane * capacity
    inside = (local >= 0) & (local < plane * capacity)
    base = jnp.arange(z_count, dtype=jnp.int32)[:, None, None] * capacity
    target = jnp.where(inside, local // capacity * share + base + local % capacity, -1)
    target_t = target.transpose(1, 0, 2).reshape(top_count, z_count * tok)
    target = target_t.T
    weight = infos[:, top_count:].transpose(0, 2, 1).reshape(z_count * tok, top_count)
    select, weigh = False, 0.0
    for j in range(top_count):
        select = select | (slot_ids[:, None] == target_t[j][None, :])
        weigh = weigh + jnp.where(target[:, j, None] == slot_ids[None, :], weight[:, j, None], 0.0)
    select, weigh = select.astype(jnp.bfloat16), weigh.astype(jnp.bfloat16)
    wide = width // CHUNKS
    last = z_count - 1
    bf, f32 = jnp.bfloat16, jnp.float32
    vmem = pl.BlockSpec(memory_space=pltpu.VMEM)
    hbm = pl.BlockSpec(memory_space=pl.ANY)
    dma = pltpu.SemaphoreType.DMA
    slab = pltpu.VMEM((CHUNKS, plane * share, wide), bf)
    hop = pltpu.VMEM((CHUNKS, last, tok, wide), bf)
    return pl.pallas_call(
        lambda *refs: experts_kernel(z_count, x_count, tp_count, *refs),
        out_shape=jax.ShapeDtypeStruct((tok, width), bf),
        in_specs=[vmem] * 4 + [hbm] * 3,
        out_specs=vmem,
        scratch_shapes=[
            pltpu.VMEM((width, hidden), bf),
            pltpu.VMEM((width, hidden), bf),
            pltpu.VMEM((hidden, width), bf),
            hop,
            slab,
            slab,
            pltpu.VMEM((plane * share, hidden), f32),
            pltpu.VMEM((plane * share, hidden), f32),
            pltpu.VMEM((plane * share, hidden), bf),
            slab,
            slab,
            pltpu.VMEM((CHUNKS, z_count * tok, wide), f32),
            hop,
            hop,
            hop,
            hop,
            dma((3,)),
            dma((CHUNKS, 2, last)),
            dma((CHUNKS, last)),
            dma((CHUNKS, plane - 1)),
            dma((CHUNKS, plane - 1)),
            dma((CHUNKS, plane - 1)),
            dma((CHUNKS, plane - 1)),
            dma((CHUNKS, 2, last)),
            dma((CHUNKS, 2, last)),
        ],
        compiler_params=pltpu.CompilerParams(
            collective_id=0, has_side_effects=True, vmem_limit_bytes=65000 * 1024
        ),
        name="experts",
    )(normed, resid, select, weigh, gate, up, down)


def body(
    stream,
    projected,
    segments,
    group_weight,
    group_scale,
    out_weight,
    ffn_gain,
    routes,
    route_weights,
    expert_gate,
    expert_up,
    expert_down,
):
    halo, docs, infos = exchange(projected, segments, routes, route_weights)
    mixed = pool(projected, halo, docs, group_weight.shape[1])
    resid, normed = mixer(mixed, stream, group_weight, group_scale, out_weight, ffn_gain)
    return run_experts(
        normed, resid, infos, expert_gate[0], expert_up[0], expert_down[0]
    )


def solution(mesh):
    in_specs = (
        P(("sp", "tp"), None),
        P("sp", "tp"),
        P("sp"),
        P(),
        P(),
        P(),
        P(),
        P(("sp", "tp"), None),
        P(("sp", "tp"), None),
        P(("sp", "tp"), None, None),
        P(("sp", "tp"), None, None),
        P(("sp", "tp"), None, None),
    )
    out_specs = P(("sp", "tp"), None)
    return jax.shard_map(body, mesh=mesh, in_specs=in_specs, out_specs=out_specs, check_vma=False)
```
